32 devices in a mesh: grp: 2 (over y), st: 8 (over z, core), tp: 2 (over x).
Axes of the slice: x: 2, y: 2, z: 4, core: 2. Of those that a mesh axis runs over, the one named last changes fastest.
Arguments:
- tokens: bfloat16 [8192, 2048], P(('grp', 'st')), parts along dimension 0, may hold values from -6 to 6
- owners: int32 [128, 4], P(('grp', 'st')), parts along dimension 0, may hold values from 0 to 7, all different within a row; in each aligned block of 8 rows (0 to 7, 8 to 15, ...) at most 8 rows name the same one
- entries: int32 [128, 4], P(('grp', 'st')), parts along dimension 0, may hold values from 0 to 15
- store: bfloat16 [256, 64, 2048], P(('grp', 'st')), parts along dimension 0, may hold values from -600 to 600
- mixer_query_weight: bfloat16 [2048, 1024], P(None, 'tp'), may hold values from -0.125 to 0.125
- mixer_key_weight: bfloat16 [2048, 1024], P(None, 'tp'), may hold values from -0.125 to 0.125
- mixer_value_weight: bfloat16 [2048, 1024], P(None, 'tp'), may hold values from -0.125 to 0.125
- strength_weight: bfloat16 [2048, 8], P(None, 'tp'), may hold values from -0.125 to 0.125
- decay_weight: bfloat16 [2048, 8], P(None, 'tp'), may hold values from -0.125 to 0.125
- head_decay_rate: float32 [8], P('tp'), may hold values from 0.003 to 0.15
- extra_forgetting_exponent: float32 [8192, 8], P(('grp', 'st'), 'tp'), parts along dimension 0, may hold values from -0.7 to 0
- output_norm_gain: float32 [128], replicated, may hold values from 0.1 to 1.9
- retrieval_query_weight: bfloat16 [2048, 1024], P(None, 'tp'), may hold values from -0.125 to 0.125
- passage_key_weight: bfloat16 [2048, 1024], P(None, 'tp'), may hold values from -0.125 to 0.125
- passage_value_weight: bfloat16 [2048, 1024], P(None, 'tp'), may hold values from -0.125 to 0.125
- retrieval_gate_weight: bfloat16 [2048, 8], P(None, 'tp'), may hold values from -0.125 to 0.125
Outputs:
- mixed: bfloat16 [8192, 1024], P(('grp', 'st'), 'tp'), parts along dimension 0
The draws below stay inside these ranges and needn't reach their ends.
There are 2 independent parts, one for each index of `grp`. The reference program is written for one: setup_inputs(seed, part) draws one part's arguments, and reference() takes and returns one part's arrays. A program takes and returns all parts, laid end to end along the dimension named above; an argument that names none is the same for every part. Nothing has to cross between parts.
Inputs may be any that keep to these rules, and one draw needn't show every extreme that they name: `owners`: each row names 4 different values; the rows of one device name no value more than 8 times, a bound that some device reaches; every value is named by some row.
All inputs are finite; a program needn't handle non-finite values.
Results may differ from the reference program's by a relative error of at most 0.015.
The reference program's roundings to bfloat16 on the way count: a program that leaves them out, or rounds other values in their place, can miss the bound.
Values may be sent and summed in bfloat16 or wider, within the bound.
A program may use at most 128 MiB of HBM per device.

```python
import math
import jax
import jax.numpy as jnp
import numpy as np
from jax import lax

D = 2048
ATTENTION_GROUPS = 8
FEATURE_WIDTH = 128
STREAM_LENGTH = 512
PASS_DEV = 16
BLOCK_TOKENS = 64
PER_BLOCK = 4
PASS_LEN = 64
POSITIONS_ALL = 4096
BLK_DEV = 8
BLOCKS = 64
PASSAGES = 128
CAP = 8
N_ST = 8


def draw_store(key, part):
    base_key = jax.random.fold_in(key, 0)
    shape = (PASSAGES, PASS_LEN, D)
    values = jnp.clip(jax.random.normal(base_key, shape, jnp.float32), -6.0, 6.0)
    return values.astype(jnp.bfloat16)


def draw_extra_forgetting_exponent(key, part):
    where_key, depth_key = jax.random.split(key, 2)
    shape = (POSITIONS_ALL, ATTENTION_GROUPS)
    struck = jax.random.uniform(where_key, shape, jnp.float32) < 1.0 / 128.0
    depth = jnp.log(jax.random.uniform(depth_key, shape, jnp.float32, 0.5, 0.8))
    return jnp.where(struck, depth, 0.0).astype(jnp.float32)


def touch_ends(values, key, low, largest):
    longest = values.shape.index(max(values.shape))
    spots = []
    for shift in (0, 1):
        where = [jax.random.randint(jax.random.fold_in(key, axis), (), 0, length) for axis, length in enumerate(values.shape)]
        where[longest] = (where[longest] + shift) % values.shape[longest]
        spots.append(tuple(where))
    return values.at[spots[0]].set(low).at[spots[1]].set(largest)


def block_scale(rng, extent, cuts, least, top_value):
    loudness = 1.0
    for position, blocks in cuts:
        steps = jax.random.uniform(jax.random.fold_in(jax.random.fold_in(rng, 6), position), (blocks,), jnp.float32, least / len(cuts), top_value / len(cuts))
        loudness = loudness * jnp.repeat(jnp.exp(steps), extent[position] // blocks).reshape((-1,) + (1,) * (len(extent) - 1 - position))
    return loudness


def deal_out(key, own, number, rows, number_of, top, most, lean):
    sequence = jax.random.permutation(key, number_of)
    heavy_load, common = portions_of(number_of, rows * top, most, lean, True), portions_of(number_of, rows * top, most, lean, False)
    places = jnp.arange(number_of)

    def named(tallies, offset_by):
        used = int((tallies > 0).sum())
        fixed = max(1, used // 4)
        moved = fixed + (places - fixed + offset_by * (used - fixed)) % max(1, number_of - fixed)
        return jnp.zeros((number_of,), jnp.int32).at[sequence[jnp.where(places < fixed, places, moved)]].set(jnp.asarray(tallies, jnp.int32))

    tallies = jnp.where(number % 4 == 0, named(heavy_load, number // 4), named(common, number - number // 4 - 1))
    mixed = jax.random.permutation(jax.random.fold_in(own, 3), number_of)
    donor, taker = mixed[0:number_of // 2 * 2:2], mixed[1:number_of // 2 * 2:2]
    room = jnp.minimum(tallies[donor] - 1, most - tallies[taker]) // 2
    room = jnp.where((donor == sequence[0]) | (taker == sequence[0]) | (tallies[taker] == 0), 0, jnp.maximum(room, 0))
    moved = jax.random.randint(jax.random.fold_in(own, 4), (number_of // 2,), 0, 1 << 20) % (room + 1)
    tallies = tallies.at[donor].add(-moved).at[taker].add(moved)
    members = jnp.searchsorted(jnp.cumsum(tallies), jnp.arange(rows * top), side="right").astype(jnp.int32)
    listing = members.reshape(top, rows).T
    listing = listing[jax.random.permutation(jax.random.fold_in(own, 1), rows)]
    offset_by = jax.random.randint(jax.random.fold_in(own, 2), (rows, 1), 0, top)
    return jnp.take_along_axis(listing, (jnp.arange(top)[None, :] + offset_by) % top, axis=1)


def portions_of(number_of, total, bound, lean, full):
    loads = [(1 << 20) // math.isqrt(standing ** lean) + 1 for standing in range(1, number_of + 1)]
    largest = bound if full else min(bound, max(-(-total // number_of), total * loads[0] // sum(loads)))
    least = 1 if total - largest >= number_of - 1 else 0
    counts, rest = [largest] + [least] * (number_of - 1), total - largest - least * (number_of - 1)
    while rest > 0:
        candidates = [i for i in range(1, number_of) if counts[i] < largest] or [i for i in range(1, number_of) if counts[i] < bound]
        pool, remaining = sum([loads[i] for i in candidates]), rest
        for i in candidates:
            addition = min(bound - counts[i], max(1, remaining * loads[i] // pool), rest)
            counts[i] = counts[i] + addition
            rest = rest - addition
    return np.array(counts)


def scatter_about(stream_key, extent, deviation, reach, shards=(), kind=jnp.bfloat16):
    gain = block_scale(stream_key, extent, shards, -0.22, 0.18) if shards else 1.0
    values = jax.random.normal(stream_key, extent, jnp.float32) * deviation * gain
    return jnp.minimum(jnp.maximum(values, -reach), reach).astype(kind)


def setup_inputs(seed: int = 0, part: int = 0) -> dict:
    keys = jax.random.split(jax.random.key(seed), 17)
    own_keys = jax.random.split(jax.random.fold_in(keys[16], part), 17)
    tokens = scatter_about(own_keys[0], (POSITIONS_ALL, D), 1.0, 6.0, ((0, 8),))
    owners_keys = jax.random.split(jax.random.fold_in(own_keys[1], 1), BLOCKS // BLK_DEV)
    owners_turns = jax.random.permutation(jax.random.fold_in(own_keys[1], 3), BLOCKS // BLK_DEV)
    owners = jax.vmap(lambda own, number: deal_out(jax.random.fold_in(own_keys[1], 2), own, number, BLK_DEV, N_ST, PER_BLOCK, CAP, 2))(owners_keys, owners_turns).reshape((BLOCKS, PER_BLOCK))
    entries = touch_ends(jax.random.randint(own_keys[2], (BLOCKS, PER_BLOCK), 0, PASS_DEV), jax.random.fold_in(own_keys[2], 1), 0, PASS_DEV - 1).astype(jnp.int32)
    store = draw_store(jax.random.fold_in(jax.random.fold_in(keys[16], part), 71), part)
    mixer_query_weight = scatter_about(keys[4], (D, ATTENTION_GROUPS * FEATURE_WIDTH), D ** -0.5, 0.125, ((1, 2),))
    mixer_key_weight = scatter_about(keys[5], (D, ATTENTION_GROUPS * FEATURE_WIDTH), D ** -0.5, 0.125, ((1, 2),))
    mixer_value_weight = scatter_about(keys[6], (D, ATTENTION_GROUPS * FEATURE_WIDTH), D ** -0.5, 0.125, ((1, 2),))
    strength_weight = scatter_about(keys[7], (D, ATTENTION_GROUPS), D ** -0.5, 0.125, ((1, 2),))
    decay_weight = scatter_about(keys[8], (D, ATTENTION_GROUPS), D ** -0.5, 0.125, ((1, 2),))
    head_decay_rate = jnp.clip(jnp.exp(math.log(0.15) - 3.912023 * jax.random.uniform(keys[9], (ATTENTION_GROUPS,), jnp.float32) ** block_scale(keys[9], (ATTENTION_GROUPS,), ((0, 2),), -0.2, 0.2)), 0.003, 0.15)
    extra_forgetting_exponent = draw_extra_forgetting_exponent(jax.random.fold_in(jax.random.fold_in(keys[16], part), 71), part)
    output_norm_gain = jnp.clip(1.0 + 0.18 * jax.random.normal(keys[11], (FEATURE_WIDTH,), jnp.float32), 0.1, 1.9)
    retrieval_query_weight = scatter_about(keys[12], (D, ATTENTION_GROUPS * FEATURE_WIDTH), D ** -0.5, 0.125, ((1, 2),))
    passage_key_weight = scatter_about(keys[13], (D, ATTENTION_GROUPS * FEATURE_WIDTH), D ** -0.5, 0.125, ((1, 2),))
    passage_value_weight = scatter_about(keys[14], (D, ATTENTION_GROUPS * FEATURE_WIDTH), D ** -0.5, 0.125, ((1, 2),))
    retrieval_gate_weight = scatter_about(keys[15], (D, ATTENTION_GROUPS), D ** -0.5, 0.125, ((1, 2),))
    return {"tokens": tokens, "owners": owners, "entries": entries, "store": store, "mixer_query_weight": mixer_query_weight, "mixer_key_weight": mixer_key_weight, "mixer_value_weight": mixer_value_weight, "strength_weight": strength_weight, "decay_weight": decay_weight, "head_decay_rate": head_decay_rate, "extra_forgetting_exponent": extra_forgetting_exponent, "output_norm_gain": output_norm_gain, "retrieval_query_weight": retrieval_query_weight, "passage_key_weight": passage_key_weight, "passage_value_weight": passage_value_weight, "retrieval_gate_weight": retrieval_gate_weight}


eps = 1e-06

def matmul_high(left, right):
    return jnp.einsum('...ij,...jk->...ik', left, right, precision=lax.Precision.HIGHEST)

def unit_lower_inverse(strict_part):
    size = strict_part.shape[-1]
    ident = jnp.eye(size, dtype=jnp.float32)
    inverse = ident - strict_part
    power = strict_part
    for level in range(size.bit_length() - 2):
        power = matmul_high(power, power)
        inverse = matmul_high(inverse, ident + power)
    return inverse

def delta_rule(queries, keys_in, values_in, decay_logarithm, strength, block_slice):
    length, heads, width = queries.shape
    count = length // block_slice

    def split(array):
        return array.reshape(count, block_slice, heads, array.shape[-1]).transpose(0, 2, 1, 3)
    q_blk = split(queries)
    k_blk = split(keys_in)
    v_blk = split(values_in)
    decay_blk = decay_logarithm.reshape(count, block_slice, heads).transpose(0, 2, 1)
    beta_blk = strength.reshape(count, block_slice, heads).transpose(0, 2, 1)
    cumul = jnp.cumsum(decay_blk, axis=-1)
    lower = jnp.tril(jnp.ones((block_slice, block_slice), bool))
    strict = jnp.tril(jnp.ones((block_slice, block_slice), bool), -1)
    spread = cumul[..., :, None] - cumul[..., None, :]
    damping = jnp.where(lower, jnp.exp(jnp.where(lower, spread, 0.0)), 0.0)
    k_beta = k_blk * beta_blk[..., None]
    inner = jnp.where(strict, matmul_high(k_beta, jnp.swapaxes(k_blk, -1, -2)) * damping, 0.0)
    inverse = unit_lower_inverse(inner)
    fresh_base = matmul_high(inverse, v_blk * beta_blk[..., None])
    key_mix = matmul_high(inverse, k_beta * jnp.exp(cumul)[..., None])
    within = jnp.where(lower, matmul_high(q_blk, jnp.swapaxes(k_blk, -1, -2)) * damping, 0.0)
    q_decayed = q_blk * jnp.exp(cumul)[..., None]
    k_tail = k_blk * jnp.exp(cumul[..., -1:] - cumul)[..., None]
    carry_decay = jnp.exp(cumul[..., -1])

    def advance(state, pieces):
        q_part, k_part, base_part, mix_part, within_part, decay_part = pieces
        fresh = base_part - matmul_high(mix_part, state)
        result = matmul_high(q_part, state) + matmul_high(within_part, fresh)
        state = state * decay_part[:, None, None] + matmul_high(jnp.swapaxes(k_part, -1, -2), fresh)
        return (state, result)
    start = jnp.zeros((heads, width, values_in.shape[-1]), jnp.float32)
    final, outputs = lax.scan(advance, start, (q_decayed, k_tail, fresh_base, key_mix, within, carry_decay))
    return outputs.transpose(0, 2, 1, 3).reshape(length, heads, values_in.shape[-1])

def mixer_head_outputs(tokens, mixer_query_weight, mixer_key_weight, mixer_value_weight, strength_weight, decay_weight, head_decay_rate, extra_forgetting_exponent, output_norm_gain, block_slice):
    heads = head_decay_rate.shape[0]
    head_dim = output_norm_gain.shape[0]
    length = tokens.shape[0]

    def project(weight):
        rounded = jnp.dot(tokens, weight, preferred_element_type=jnp.float32).astype(jnp.bfloat16)
        return lax.optimization_barrier(rounded).astype(jnp.float32).reshape(length, heads, head_dim)

    def unit_rows(array):
        return array * lax.rsqrt(lax.optimization_barrier(jnp.sum(array * array, axis=-1, keepdims=True)) + eps)
    queries = unit_rows(project(mixer_query_weight)) * head_dim ** (-0.5)
    keys_in = unit_rows(project(mixer_key_weight))
    values_in = project(mixer_value_weight)
    strength = jax.nn.sigmoid(jnp.dot(tokens, strength_weight, preferred_element_type=jnp.float32))
    decay_logarithm = -head_decay_rate[None, :] * jax.nn.softplus(jnp.dot(tokens, decay_weight, preferred_element_type=jnp.float32)) + extra_forgetting_exponent
    recur = delta_rule(queries, keys_in, values_in, decay_logarithm, strength, block_slice)
    return recur * lax.rsqrt(lax.optimization_barrier(jnp.mean(recur * recur, axis=-1, keepdims=True)) + eps) * output_norm_gain

def reference(tokens, owners, entries, store, mixer_query_weight, mixer_key_weight, mixer_value_weight, strength_weight, decay_weight, head_decay_rate, extra_forgetting_exponent, output_norm_gain, retrieval_query_weight, passage_key_weight, passage_value_weight, retrieval_gate_weight):
    stream_group = tokens.reshape(N_ST, STREAM_LENGTH, D)
    forgetting_spikes = extra_forgetting_exponent.reshape(N_ST, STREAM_LENGTH, ATTENTION_GROUPS)

    def lone_stream(pair):
        return mixer_head_outputs(pair[0], mixer_query_weight, mixer_key_weight, mixer_value_weight, strength_weight, decay_weight, head_decay_rate, pair[1], output_norm_gain, BLOCK_TOKENS)
    rescaled_result = lax.map(lone_stream, (stream_group, forgetting_spikes)).reshape(POSITIONS_ALL, ATTENTION_GROUPS, FEATURE_WIDTH)
    flat_store = store.reshape(PASSAGES * PASS_LEN, D)
    pass_key = jnp.dot(flat_store, passage_key_weight, preferred_element_type=jnp.float32).astype(jnp.bfloat16).reshape(PASSAGES, PASS_LEN, ATTENTION_GROUPS * FEATURE_WIDTH)
    pass_value = jnp.dot(flat_store, passage_value_weight, preferred_element_type=jnp.float32).astype(jnp.bfloat16).reshape(PASSAGES, PASS_LEN, ATTENTION_GROUPS * FEATURE_WIDTH)
    passage = (owners.astype(jnp.int32) * PASS_DEV + entries.astype(jnp.int32)).astype(jnp.int32)
    keys_read = pass_key[passage].reshape(BLOCKS, PER_BLOCK * PASS_LEN, ATTENTION_GROUPS, FEATURE_WIDTH)
    values_read = pass_value[passage].reshape(BLOCKS, PER_BLOCK * PASS_LEN, ATTENTION_GROUPS, FEATURE_WIDTH)
    rquery = jnp.dot(tokens, retrieval_query_weight, preferred_element_type=jnp.float32).astype(jnp.bfloat16).reshape(BLOCKS, BLOCK_TOKENS, ATTENTION_GROUPS, FEATURE_WIDTH)
    scores = jnp.einsum('bqhd,bkhd->bhqk', rquery.astype(jnp.float32), keys_read.astype(jnp.float32)) * FEATURE_WIDTH ** (-0.5)
    peak = lax.optimization_barrier(jnp.max(scores, axis=-1, keepdims=True))
    expo = jnp.exp(scores - peak)
    weights = (expo / lax.optimization_barrier(jnp.sum(expo, axis=-1, keepdims=True))).astype(jnp.bfloat16)
    retrieved = jnp.einsum('bhqk,bkhd->bqhd', weights.astype(jnp.float32), values_read.astype(jnp.float32)).reshape(POSITIONS_ALL, ATTENTION_GROUPS, FEATURE_WIDTH)
    rgate = jax.nn.sigmoid(jnp.dot(tokens, retrieval_gate_weight, preferred_element_type=jnp.float32))
    mixed = rescaled_result + rgate[..., None] * retrieved
    return mixed.reshape(POSITIONS_ALL, ATTENTION_GROUPS * FEATURE_WIDTH).astype(jnp.bfloat16)
```

```python
import functools

import jax
import jax.numpy as jnp
from jax import lax
from jax.experimental import pallas as pl
from jax.experimental.pallas import tpu as pltpu
from jax.sharding import PartitionSpec as P

BLOCK_TOKENS = 64
EPS = 1e-06
MISSING = -1e30
F32 = jnp.float32
BF16 = jnp.bfloat16


def dot_nt(left, right):
    return lax.dot_general(left, right, (((1,), (1,)), ((), ())), preferred_element_type=F32)


def dot_tn(left, right):
    return lax.dot_general(left, right, (((0,), (0,)), ((), ())), preferred_element_type=F32)


def dot_nn(left, right):
    return jnp.dot(left.astype(BF16), right.astype(BF16), preferred_element_type=F32)


def attend_kernel(units, head_dim, passage_rows, blocks, sel_ref, core_ref, *refs):
    queries = refs[:units]
    k_own, v_own, k_sib, v_sib = refs[units : units + 4]
    outs = refs[units + 4 :]
    heads = k_sib.shape[1] // head_dim
    length = queries[0].shape[0]
    scale = head_dim ** (-0.5)
    for unit in range(units):
        q_ref, o_ref = queries[unit], outs[unit]
        stats = []
        for block in range(blocks):
            base = (unit * blocks + block) * 2
            mine, other = sel_ref[base], sel_ref[base + 1]
            row_own = pl.multiple_of(jnp.maximum(mine, 0) * passage_rows, passage_rows)
            row_sib = pl.multiple_of(jnp.maximum(other, 0) * passage_rows, passage_rows)
            bias_own = jnp.where(mine >= 0, 0.0, MISSING).astype(F32)
            bias_sib = jnp.where(other >= 0, 0.0, MISSING).astype(F32)
            rows = slice(block * BLOCK_TOKENS, (block + 1) * BLOCK_TOKENS)
            line = []
            for head in range(heads):
                cols = slice(head * head_dim, (head + 1) * head_dim)
                query = q_ref[rows, cols]
                own = dot_nt(k_own[pl.ds(row_own, passage_rows), cols], query) * scale + bias_own
                sib = dot_nt(k_sib[pl.ds(row_sib, passage_rows), cols], query) * scale + bias_sib
                peak = jnp.maximum(
                    jnp.max(own, axis=0, keepdims=True), jnp.max(sib, axis=0, keepdims=True)
                )
                e_own = jnp.exp(own - peak)
                e_sib = jnp.exp(sib - peak)
                total = jnp.sum(e_own, axis=0, keepdims=True) + jnp.sum(
                    e_sib, axis=0, keepdims=True
                )
                inv = 1.0 / total
                result = dot_tn(
                    (e_own * inv).astype(BF16), v_own[pl.ds(row_own, passage_rows), cols]
                ) + dot_tn((e_sib * inv).astype(BF16), v_sib[pl.ds(row_sib, passage_rows), cols])
                o_ref[rows, cols] = result.astype(BF16)
                line.append(peak + jnp.log(total))
            stats.append(jnp.concatenate(line, axis=0))
        store_stats(o_ref, jnp.concatenate(stats, axis=1), length)


def store_stats(o_ref, lse, length):
    heads = lse.shape[0]
    width = o_ref.shape[1]
    high = lse.astype(BF16).astype(F32)
    mid = (lse - high).astype(BF16).astype(F32)
    low = lse - high - mid
    pad = jnp.zeros((16 - 3 * heads, length), F32)
    pieces = jnp.concatenate([high, mid, low, pad], axis=0).astype(BF16)
    for part in range(length // width):
        o_ref[length + 16 * part : length + 16 * (part + 1), :] = pieces[
            :, part * width : (part + 1) * width
        ]


def load_stats(ref, length, heads):
    width = ref.shape[1]
    parts = [
        ref[length + 16 * part : length + 16 * (part + 1), :].astype(F32)
        for part in range(length // width)
    ]
    pieces = jnp.concatenate(parts, axis=1)
    return pieces[:heads] + pieces[heads : 2 * heads] + pieces[2 * heads : 3 * heads]


def blend(refs, length, heads, head_dim):
    stats = [load_stats(ref, length, heads) for ref in refs]
    peak = functools.reduce(jnp.maximum, stats)
    expo = [jnp.exp(stat - peak) for stat in stats]
    total = functools.reduce(jnp.add, expo)
    inv = 1.0 / total
    lse = peak + jnp.log(total)
    shares = [
        jnp.transpose(jnp.concatenate([e * inv] + [jnp.zeros((8 - heads, length), F32)], axis=0))
        for e in expo
    ]
    results = []
    for head in range(heads):
        cols = slice(head * head_dim, (head + 1) * head_dim)
        results.append(
            functools.reduce(
                jnp.add,
                [
                    ref[:length, cols].astype(F32) * share[:, head : head + 1]
                    for ref, share in zip(refs, shares)
                ],
            )
        )
    return results, lse


def merge_kernel(length, head_dim, final, *refs):
    inputs, o_ref = refs[:-1], refs[-1]
    heads = o_ref.shape[1] // head_dim
    results, lse = blend(inputs, length, heads, head_dim)
    for head, result in enumerate(results):
        o_ref[:length, head * head_dim : (head + 1) * head_dim] = result.astype(BF16)
    if not final:
        store_stats(o_ref, lse, length)


def merge(parts, length, head_dim, final=False):
    shape = (length, parts[0].shape[1]) if final else parts[0].shape
    return pl.pallas_call(
        functools.partial(merge_kernel, length, head_dim, final),
        out_shape=jax.ShapeDtypeStruct(shape, BF16),
        cost_estimate=pl.CostEstimate(flops=2_000_000, bytes_accessed=3_000_000, transcendentals=0),
        name="merge",
    )(*parts)


def attend(units, sel, core, keys, values, keys_sib, values_sib, head_dim, passage_rows):
    length, half = units[0].shape
    blocks = length // BLOCK_TOKENS
    rows = keys.shape[0]
    packed = length + 16 * (length // half)
    whole = lambda shape: pl.BlockSpec(shape, lambda i, s, c: (0, 0))
    mine = pl.BlockSpec((rows, half), lambda i, s, c: (0, c[0]))
    return pl.pallas_call(
        functools.partial(attend_kernel, len(units), head_dim, passage_rows, blocks),
        out_shape=[jax.ShapeDtypeStruct((packed, half), BF16)] * len(units),
        grid_spec=pltpu.PrefetchScalarGridSpec(
            num_scalar_prefetch=2,
            grid=(1,),
            in_specs=[whole((length, half))] * len(units)
            + [mine, mine, whole((rows, half)), whole((rows, half))],
            out_specs=[whole((packed, half))] * len(units),
        ),
        cost_estimate=pl.CostEstimate(
            flops=2_000_000_000 * len(units), bytes_accessed=4_000_000, transcendentals=0
        ),
        name="attend",
    )(sel, core, *units, keys, values, keys_sib, values_sib)


def delta_kernel(pack, chunk, q_ref, k_ref, v_ref, gate_ref, extra_ref, rate_ref, gain_ref, o_ref):
    length, width = q_ref.shape
    head_dim = gain_ref.shape[1]
    heads = width // head_dim
    packs = length // pack
    scale = head_dim ** (-0.5)
    row = lax.broadcasted_iota(jnp.int32, (pack, pack), 0)
    col = lax.broadcasted_iota(jnp.int32, (pack, pack), 1)
    same = (row // chunk) == (col // chunk)
    lower = same & (row >= col)
    strict = same & (row > col)
    ident = jnp.where(row == col, 1.0, 0.0).astype(F32)
    tri = jnp.where(lower, 1.0, 0.0).astype(F32)
    tail = jnp.where(same, 1.0, 0.0).astype(F32)
    gates = gate_ref[...]
    beta_all = jax.nn.sigmoid(gates[:, :heads])
    raw = gates[:, heads : 2 * heads]
    softplus = jnp.maximum(raw, 0.0) + jnp.log1p(jnp.exp(-jnp.abs(raw)))
    decay_all = -rate_ref[...] * softplus + extra_ref[...]
    gain = gain_ref[...]
    work = []
    for half in range(packs):
        rows = slice(half * pack, (half + 1) * pack)
        decay = jnp.concatenate([decay_all[rows], jnp.zeros((pack, 128 - heads), F32)], axis=1)
        cum = jnp.dot(tri, decay, precision=lax.Precision.HIGHEST, preferred_element_type=F32)
        ends = jnp.dot(tail, decay, precision=lax.Precision.HIGHEST, preferred_element_type=F32)
        cum_t = jnp.transpose(cum)
        for head in range(heads):
            cols = slice(head * head_dim, (head + 1) * head_dim)
            q, k, v = q_ref[rows, cols], k_ref[rows, cols], v_ref[rows, cols]
            q32, k32 = q.astype(F32), k.astype(F32)
            qn = q32 * (lax.rsqrt(jnp.sum(q32 * q32, axis=1, keepdims=True) + EPS) * scale)
            kn = k32 * lax.rsqrt(jnp.sum(k32 * k32, axis=1, keepdims=True) + EPS)
            beta = beta_all[rows, head : head + 1]
            c_col = cum[:, head : head + 1]
            spread = c_col - cum_t[head : head + 1, :]
            damp = jnp.where(lower, jnp.exp(jnp.where(lower, spread, 0.0)), 0.0)
            kb = kn.astype(BF16)
            inner = jnp.where(strict, dot_nt(kb, kb) * damp * beta, 0.0)
            within = (dot_nt(qn.astype(BF16), kb) * damp).astype(BF16)
            inverse = ident
            size = 1
            while size < chunk:
                cut = ((row // (2 * size)) == (col // (2 * size))) & ((row // size) != (col // size))
                piece = jnp.where(cut, inner, 0.0)
                if size == 1:
                    inverse = ident - piece
                else:
                    inverse = inverse - dot_nn(dot_nn(inverse, piece), inverse)
                size *= 2
            grow = jnp.exp(c_col)
            sides = jnp.concatenate([v.astype(F32) * beta, kn * (beta * grow)], axis=1)
            mixed = dot_nn(inverse, sides)
            base, key_mix = mixed[:, :head_dim], mixed[:, head_dim:]
            q_dec = qn * grow
            k_tail = kn * jnp.exp(ends[:, head : head + 1] - c_col)
            work.append(
                (
                    base,
                    key_mix.astype(BF16),
                    q_dec.astype(BF16),
                    jnp.transpose(k_tail).astype(BF16),
                    within,
                    jnp.exp(ends[:, head : head + 1]),
                )
            )
    state = [jnp.zeros((head_dim, head_dim), F32) for _ in range(heads)]
    for half in range(packs):
        fresh_parts = [[] for _ in range(heads)]
        cross_parts = [[] for _ in range(heads)]
        for step in range(pack // chunk):
            rows = slice(step * chunk, (step + 1) * chunk)
            for head in range(heads):
                base, key_mix, q_dec, k_tail, _, carry = work[half * heads + head]
                stacked = jnp.concatenate([key_mix[rows], q_dec[rows]], axis=0)
                read = jnp.dot(stacked, state[head].astype(BF16), preferred_element_type=F32)
                fresh = (base[rows] - read[:chunk]).astype(BF16)
                cross_parts[head].append(read[chunk:])
                fresh_parts[head].append(fresh)
                kept = carry[step * chunk : step * chunk + 1, :]
                state[head] = state[head] * kept + jnp.dot(
                    k_tail[:, rows], fresh, preferred_element_type=F32
                )
        for head in range(heads):
            within = work[half * heads + head][4]
            result = jnp.concatenate(cross_parts[head], axis=0) + jnp.dot(
                within, jnp.concatenate(fresh_parts[head], axis=0), preferred_element_type=F32
            )
            norm = lax.rsqrt(jnp.mean(result * result, axis=1, keepdims=True) + EPS)
            o_ref[half * pack : (half + 1) * pack, head * head_dim : (head + 1) * head_dim] = (
                result * norm * gain
            )


def delta(q, k, v, gates, extra, rate, gain, pack):
    return pl.pallas_call(
        functools.partial(delta_kernel, pack, BLOCK_TOKENS),
        out_shape=jax.ShapeDtypeStruct(q.shape, F32),
        cost_estimate=pl.CostEstimate(
            flops=12_000_000_000, bytes_accessed=4_000_000, transcendentals=0
        ),
        name="delta",
    )(q, k, v, gates, extra, rate[None, :], gain[None, :])


def final_kernel(head_dim, heads, core_ref, normed_ref, gate_ref, other_ref, *refs):
    parts, o_ref = refs[:-1], refs[-1]
    length, half = other_ref.shape
    here = heads // 2
    core = core_ref[0]
    gates = jax.nn.sigmoid(gate_ref[...][:, 2 * heads : 3 * heads])
    results, _ = blend(parts, length, here, head_dim)
    for which in range(2):
        for head in range(here):
            side = core if which == 0 else 1 - core
            start = pl.multiple_of(side * half + head * head_dim, head_dim)
            cols = pl.ds(start, head_dim)
            gate = jnp.where(
                side == 0, gates[:, head : head + 1], gates[:, here + head : here + head + 1]
            )
            if which == 0:
                value = results[head]
            else:
                value = other_ref[:, head * head_dim : (head + 1) * head_dim].astype(F32)
            o_ref[:, cols] = (normed_ref[:, cols] + gate * value).astype(BF16)


def finish(core, normed, gates, other, parts, head_dim, heads):
    return pl.pallas_call(
        functools.partial(final_kernel, head_dim, heads),
        out_shape=jax.ShapeDtypeStruct(normed.shape, BF16),
        in_specs=[pl.BlockSpec(memory_space=pltpu.SMEM)]
        + [pl.BlockSpec(memory_space=pltpu.VMEM)] * (3 + len(parts)),
        name="finish",
    )(core, normed, gates, other, *parts)


def per_device(
    tokens,
    owners,
    entries,
    store,
    mixer_query_weight,
    mixer_key_weight,
    mixer_value_weight,
    strength_weight,
    decay_weight,
    head_decay_rate,
    extra_forgetting_exponent,
    output_norm_gain,
    retrieval_query_weight,
    passage_key_weight,
    passage_value_weight,
    retrieval_gate_weight,
):
    heads = head_decay_rate.shape[0]
    head_dim = output_norm_gain.shape[0]
    length = tokens.shape[0]
    devices = lax.axis_size("st")
    chips = devices // 2
    blocks = owners.shape[0]
    passage_rows = store.shape[1]
    half = heads * head_dim // 2
    me = lax.axis_index("st")
    core, chip = me % 2, me // 2
    swap = [(i, i ^ 1) for i in range(devices)]
    right = [(i, (i + 2) % devices) for i in range(devices)]
    left = [(i, (i - 2) % devices) for i in range(devices)]
    send = lambda array, pairs: lax.ppermute(array, "st", pairs)

    def project(rows, weight):
        return jnp.dot(rows, weight, preferred_element_type=F32).astype(BF16)

    rquery = project(tokens, retrieval_query_weight)
    q_own = lax.dynamic_slice_in_dim(rquery, core * half, half, 1)
    q_sib = send(lax.dynamic_slice_in_dim(rquery, (1 - core) * half, half, 1), swap)

    wants = lax.all_gather(jnp.concatenate([owners, entries], axis=1), "st", axis=0, tiled=True)
    width = owners.shape[1]
    w_own, w_ent = wants[:, :width], wants[:, width:]

    def pick(owner):
        return jnp.sum(jnp.where(w_own == owner, w_ent + 1, 0), axis=1) - 1

    sel = jnp.stack([pick(me), pick(me ^ 1)], axis=1).reshape(chips, 2, blocks * 2)
    sel = jnp.where(core == 0, sel, sel[:, ::-1])
    sel = jnp.roll(sel, -chip, axis=0)

    reach = chips // 2
    from_left, from_right = [(q_own, q_sib)], [(q_own, q_sib)]
    for hop in range(1, reach):
        from_left.append(tuple(send(part, right) for part in from_left[-1]))
        from_right.append(tuple(send(part, left) for part in from_right[-1]))
    far_own = send(from_left[-1][0], right)
    far_sib = send(from_right[-1][1], left)

    flat_store = store.reshape(-1, store.shape[2])
    keys = project(flat_store, passage_key_weight)
    values = project(flat_store, passage_value_weight)
    away = (1 - core) * half
    keys_sib = send(lax.dynamic_slice_in_dim(keys, away, half, 1), swap)
    values_sib = send(lax.dynamic_slice_in_dim(values, away, half, 1), swap)

    core_arr = core.reshape(1).astype(jnp.int32)

    def attended(units, offsets):
        chosen = jnp.concatenate([sel[offset].reshape(-1) for offset in offsets])
        return attend(
            units, chosen, core_arr, keys, values, keys_sib, values_sib, head_dim, passage_rows
        )

    here = attended(list(from_left[0]), [0])
    to_left, to_right = {}, {}
    for hop in range(1, reach):
        res = attended(list(from_left[hop]) + list(from_right[hop]), [(-hop) % chips, hop])
        to_left[hop], to_right[hop] = res[:2], res[2:]
    far = attended([far_own, far_sib], [reach])

    q = project(tokens, mixer_query_weight)
    k = project(tokens, mixer_key_weight)
    v = project(tokens, mixer_value_weight)
    small = jnp.concatenate([strength_weight, decay_weight, retrieval_gate_weight], axis=1)
    gates = jnp.dot(tokens, small, preferred_element_type=F32)
    normed = delta(
        q, k, v, gates, extra_forgetting_exponent, head_decay_rate, output_norm_gain,
        min(4 * BLOCK_TOKENS, length),
    )

    going_right, going_left = [far[0], None], [None, far[1]]
    for hop in range(reach - 1, 0, -1):
        for going, pairs, mine in (
            (going_right, right, to_right[hop]),
            (going_left, left, to_left[hop]),
        ):
            for part in range(2):
                if going[part] is None:
                    going[part] = mine[part]
                else:
                    going[part] = merge([send(going[part], pairs), mine[part]], length, head_dim)
    ends = [
        [here[part]]
        + [send(going[part], pairs) for going, pairs in ((going_right, right), (going_left, left))
           if going[part] is not None]
        for part in range(2)
    ]
    other = send(merge(ends[1], length, head_dim, final=True), swap)
    return finish(core_arr, normed, gates, other, ends[0], head_dim, heads)


def solution(mesh):
    rows = ("grp", "st")
    return jax.shard_map(
        per_device,
        mesh=mesh,
        in_specs=(
            P(rows, None),
            P(rows, None),
            P(rows, None),
            P(rows, None, None),
            P(None, "tp"),
            P(None, "tp"),
            P(None, "tp"),
            P(None, "tp"),
            P(None, "tp"),
            P("tp"),
            P(rows, "tp"),
            P(),
            P(None, "tp"),
            P(None, "tp"),
            P(None, "tp"),
            P(None, "tp"),
        ),
        out_specs=P(rows, "tp"),
        check_vma=False,
    )
```

```python
import functools

import jax
import jax.numpy as jnp
from jax import lax
from jax.experimental import pallas as pl
from jax.experimental.pallas import tpu as pltpu
from jax.sharding import PartitionSpec as P

BLOCK_TOKENS = 64
EPS = 1e-06
MISSING = -1e30
F32 = jnp.float32
BF16 = jnp.bfloat16


def dot_nt(left, right):
    return lax.dot_general(left, right, (((1,), (1,)), ((), ())), preferred_element_type=F32)


def dot_tn(left, right):
    return lax.dot_general(left, right, (((0,), (0,)), ((), ())), preferred_element_type=F32)


def dot_nn(left, right):
    return jnp.dot(left.astype(BF16), right.astype(BF16), preferred_element_type=F32)


def attend_kernel(
    offsets, head_dim, passage_rows, blocks, chips, per_device_passages, want_ref, info_ref, *refs
):
    units = len(offsets)
    queries = refs[:units]
    k_own, v_own, k_sib, v_sib = refs[units : units + 4]
    outs = refs[units + 4 :]
    length, half = queries[0].shape
    heads = half // head_dim
    width = want_ref.shape[1]
    scale = head_dim ** (-0.5)
    core, me = info_ref[0], info_ref[1]
    chip = (me - core) // 2
    first_own = me * per_device_passages
    first_sib = (me + 1 - 2 * core) * per_device_passages

    def find(named, first):
        hit = jnp.int32(0)
        for value in named:
            inside = (value >= first) & (value < first + per_device_passages)
            hit = jnp.where(inside, value - first + 1, hit)
        row = pl.multiple_of(jnp.maximum(hit - 1, 0) * passage_rows, passage_rows)
        return row, jnp.where(hit > 0, 0.0, MISSING).astype(F32)

    nothing = jnp.zeros((BLOCK_TOKENS, head_dim), BF16)
    for unit, (hop, sibling) in enumerate(offsets):
        q_ref, o_ref = queries[unit], outs[unit]
        source = lax.rem(chip + hop + chips, chips) * 2 + (1 - core if sibling else core)
        stats = []
        for block in range(blocks):
            line = source * blocks + block
            named = [want_ref[line, place] for place in range(width)]
            row_own, bias_own = find(named, first_own)
            row_sib, bias_sib = find(named, first_sib)
            rows = slice(block * BLOCK_TOKENS, (block + 1) * BLOCK_TOKENS)
            query = q_ref[rows, :]
            spread = jnp.concatenate(
                [
                    jnp.concatenate(
                        [
                            query[:, head * head_dim : (head + 1) * head_dim]
                            if head == place
                            else nothing
                            for place in range(heads)
                        ],
                        axis=1,
                    )
                    for head in range(heads)
                ],
                axis=0,
            )
            keys = jnp.concatenate(
                [k_own[pl.ds(row_own, passage_rows), :], k_sib[pl.ds(row_sib, passage_rows), :]],
                axis=0,
            )
            values = jnp.concatenate(
                [v_own[pl.ds(row_own, passage_rows), :], v_sib[pl.ds(row_sib, passage_rows), :]],
                axis=0,
            )
            scores = dot_nt(keys, spread) * scale
            own, sib = scores[:passage_rows] + bias_own, scores[passage_rows:] + bias_sib
            peak = jnp.max(jnp.maximum(own, sib), axis=0, keepdims=True)
            e_own = jnp.exp(own - peak)
            e_sib = jnp.exp(sib - peak)
            total = jnp.sum(e_own + e_sib, axis=0, keepdims=True)
            inv = 1.0 / total
            weights = jnp.concatenate([e_own * inv, e_sib * inv], axis=0).astype(BF16)
            result = dot_tn(weights, values)
            lse = peak + jnp.log(total)
            for head in range(heads):
                cols = slice(head * head_dim, (head + 1) * head_dim)
                span = slice(head * BLOCK_TOKENS, (head + 1) * BLOCK_TOKENS)
                o_ref[rows, cols] = result[span, cols].astype(BF16)
            stats.append(
                jnp.concatenate(
                    [
                        lse[:, head * BLOCK_TOKENS : (head + 1) * BLOCK_TOKENS]
                        for head in range(heads)
                    ],
                    axis=0,
                )
            )
        store_stats(o_ref, jnp.concatenate(stats, axis=1), length)


def store_stats(o_ref, lse, length):
    heads = lse.shape[0]
    width = o_ref.shape[1]
    high = lse.astype(BF16).astype(F32)
    mid = (lse - high).astype(BF16).astype(F32)
    low = lse - high - mid
    pad = jnp.zeros((16 - 3 * heads, length), F32)
    pieces = jnp.concatenate([high, mid, low, pad], axis=0).astype(BF16)
    for part in range(length // width):
        o_ref[length + 16 * part : length + 16 * (part + 1), :] = pieces[
            :, part * width : (part + 1) * width
        ]


def load_stats(ref, length, heads):
    width = ref.shape[1]
    parts = [
        ref[length + 16 * part : length + 16 * (part + 1), :].astype(F32)
        for part in range(length // width)
    ]
    pieces = jnp.concatenate(parts, axis=1)
    return pieces[:heads] + pieces[heads : 2 * heads] + pieces[2 * heads : 3 * heads]


def blend(refs, length, heads, head_dim):
    stats = [load_stats(ref, length, heads) for ref in refs]
    peak = functools.reduce(jnp.maximum, stats)
    expo = [jnp.exp(stat - peak) for stat in stats]
    total = functools.reduce(jnp.add, expo)
    inv = 1.0 / total
    lse = peak + jnp.log(total)
    shares = [
        jnp.transpose(jnp.concatenate([e * inv] + [jnp.zeros((8 - heads, length), F32)], axis=0))
        for e in expo
    ]
    results = []
    for head in range(heads):
        cols = slice(head * head_dim, (head + 1) * head_dim)
        results.append(
            functools.reduce(
                jnp.add,
                [
                    ref[:length, cols].astype(F32) * share[:, head : head + 1]
                    for ref, share in zip(refs, shares)
                ],
            )
        )
    return results, lse


def merge_kernel(length, head_dim, final, *refs):
    inputs, o_ref = refs[:-1], refs[-1]
    heads = o_ref.shape[1] // head_dim
    results, lse = blend(inputs, length, heads, head_dim)
    for head, result in enumerate(results):
        o_ref[:length, head * head_dim : (head + 1) * head_dim] = result.astype(BF16)
    if not final:
        store_stats(o_ref, lse, length)


def merge(parts, length, head_dim, final=False):
    shape = (length, parts[0].shape[1]) if final else parts[0].shape
    return pl.pallas_call(
        functools.partial(merge_kernel, length, head_dim, final),
        out_shape=jax.ShapeDtypeStruct(shape, BF16),
        cost_estimate=pl.CostEstimate(flops=2_000_000, bytes_accessed=3_000_000, transcendentals=0),
        name="merge",
    )(*parts)


def attend(units, offsets, wants, info, keys, values, pair_sib, head_dim, passage_rows, chips):
    length, half = units[0].shape
    blocks = length // BLOCK_TOKENS
    rows = keys.shape[0]
    packed = length + 16 * (length // half)
    whole = lambda shape: pl.BlockSpec(shape, lambda i, w, c: (0, 0))
    mine = pl.BlockSpec((rows, half), lambda i, w, c: (0, c[0]))
    second = pl.BlockSpec((rows, half), lambda i, w, c: (0, 1))
    return pl.pallas_call(
        functools.partial(
            attend_kernel, offsets, head_dim, passage_rows, blocks, chips, rows // passage_rows
        ),
        out_shape=[jax.ShapeDtypeStruct((packed, half), BF16)] * len(units),
        grid_spec=pltpu.PrefetchScalarGridSpec(
            num_scalar_prefetch=2,
            grid=(1,),
            in_specs=[whole((length, half))] * len(units)
            + [mine, mine, whole((rows, half)), second],
            out_specs=[whole((packed, half))] * len(units),
        ),
        cost_estimate=pl.CostEstimate(
            flops=1_500_000_000 * len(units), bytes_accessed=4_000_000, transcendentals=0
        ),
        name="attend",
    )(wants, info, *units, keys, values, pair_sib, pair_sib)


def delta_kernel(pack, chunk, first, q_ref, k_ref, v_ref, gate_ref, extra_ref, rate_ref, gain_ref, o_ref):
    length, width = q_ref.shape
    head_dim = gain_ref.shape[1]
    heads = width // head_dim
    packs = length // pack
    scale = head_dim ** (-0.5)
    row = lax.broadcasted_iota(jnp.int32, (pack, pack), 0)
    col = lax.broadcasted_iota(jnp.int32, (pack, pack), 1)
    same = (row // chunk) == (col // chunk)
    lower = same & (row >= col)
    strict = same & (row > col)
    ident = jnp.where(row == col, 1.0, 0.0).astype(F32)
    tri = jnp.where(lower, 1.0, 0.0).astype(F32)
    tail = jnp.where(same, 1.0, 0.0).astype(F32)
    gates = gate_ref[...]
    every = rate_ref.shape[1]
    beta_all = jax.nn.sigmoid(gates[:, first : first + heads])
    raw = gates[:, every + first : every + first + heads]
    softplus = jnp.maximum(raw, 0.0) + jnp.log1p(jnp.exp(-jnp.abs(raw)))
    mine = slice(first, first + heads)
    decay_all = -rate_ref[:, mine] * softplus + extra_ref[:, mine]
    gain = gain_ref[...]
    work = []
    for half in range(packs):
        rows = slice(half * pack, (half + 1) * pack)
        decay = jnp.concatenate([decay_all[rows], jnp.zeros((pack, 128 - heads), F32)], axis=1)
        cum = jnp.dot(tri, decay, precision=lax.Precision.HIGHEST, preferred_element_type=F32)
        ends = jnp.dot(tail, decay, precision=lax.Precision.HIGHEST, preferred_element_type=F32)
        cum_t = jnp.transpose(cum)
        for head in range(heads):
            cols = slice(head * head_dim, (head + 1) * head_dim)
            q, k, v = q_ref[rows, cols], k_ref[rows, cols], v_ref[rows, cols]
            q32, k32 = q.astype(F32), k.astype(F32)
            qn = q32 * (lax.rsqrt(jnp.sum(q32 * q32, axis=1, keepdims=True) + EPS) * scale)
            kn = k32 * lax.rsqrt(jnp.sum(k32 * k32, axis=1, keepdims=True) + EPS)
            beta = beta_all[rows, head : head + 1]
            c_col = cum[:, head : head + 1]
            spread = c_col - cum_t[head : head + 1, :]
            damp = jnp.where(lower, jnp.exp(jnp.where(lower, spread, 0.0)), 0.0)
            kb = kn.astype(BF16)
            inner = jnp.where(strict, dot_nt(kb, kb) * damp * beta, 0.0)
            within = (dot_nt(qn.astype(BF16), kb) * damp).astype(BF16)
            inverse = ident
            size = 1
            while size < chunk:
                cut = ((row // (2 * size)) == (col // (2 * size))) & ((row // size) != (col // size))
                piece = jnp.where(cut, inner, 0.0)
                if size == 1:
                    inverse = ident - piece
                else:
                    inverse = inverse - dot_nn(dot_nn(inverse, piece), inverse)
                size *= 2
            grow = jnp.exp(c_col)
            sides = jnp.concatenate([v.astype(F32) * beta, kn * (beta * grow)], axis=1)
            mixed = dot_nn(inverse, sides)
            base, key_mix = mixed[:, :head_dim], mixed[:, head_dim:]
            q_dec = qn * grow
            k_tail = kn * jnp.exp(ends[:, head : head + 1] - c_col)
            work.append(
                (
                    base,
                    key_mix.astype(BF16),
                    q_dec.astype(BF16),
                    jnp.transpose(k_tail).astype(BF16),
                    within,
                    jnp.exp(ends[:, head : head + 1]),
                )
            )
    state = [jnp.zeros((head_dim, head_dim), F32) for _ in range(heads)]
    for half in range(packs):
        fresh_parts = [[] for _ in range(heads)]
        cross_parts = [[] for _ in range(heads)]
        for step in range(pack // chunk):
            rows = slice(step * chunk, (step + 1) * chunk)
            for head in range(heads):
                base, key_mix, q_dec, k_tail, _, carry = work[half * heads + head]
                stacked = jnp.concatenate([key_mix[rows], q_dec[rows]], axis=0)
                read = jnp.dot(stacked, state[head].astype(BF16), preferred_element_type=F32)
                fresh = (base[rows] - read[:chunk]).astype(BF16)
                cross_parts[head].append(read[chunk:])
                fresh_parts[head].append(fresh)
                kept = carry[step * chunk : step * chunk + 1, :]
                state[head] = state[head] * kept + jnp.dot(
                    k_tail[:, rows], fresh, preferred_element_type=F32
                )
        for head in range(heads):
            within = work[half * heads + head][4]
            result = jnp.concatenate(cross_parts[head], axis=0) + jnp.dot(
                within, jnp.concatenate(fresh_parts[head], axis=0), preferred_element_type=F32
            )
            norm = lax.rsqrt(jnp.mean(result * result, axis=1, keepdims=True) + EPS)
            o_ref[half * pack : (half + 1) * pack, head * head_dim : (head + 1) * head_dim] = (
                result * norm * gain
            )


def delta(q, k, v, gates, extra, rate, gain, pack, group, groups):
    length, width = q.shape
    half = width // groups
    first = group * (rate.shape[0] // groups)
    part = pl.BlockSpec((length, half), lambda i: (0, group))
    whole = lambda array: pl.BlockSpec(array.shape, lambda i: (0, 0))
    rate, gain = rate[None, :], gain[None, :]
    return pl.pallas_call(
        functools.partial(delta_kernel, pack, BLOCK_TOKENS, first),
        out_shape=jax.ShapeDtypeStruct((length, half), F32),
        grid=(1,),
        in_specs=[part, part, part, whole(gates), whole(extra), whole(rate), whole(gain)],
        out_specs=pl.BlockSpec((length, half), lambda i: (0, 0)),
        cost_estimate=pl.CostEstimate(
            flops=8_000_000_000, bytes_accessed=2_000_000, transcendentals=0
        ),
        name="delta",
    )(q, k, v, gates, extra, rate, gain)


def final_kernel(head_dim, heads, info_ref, low_ref, high_ref, gate_ref, other_ref, *refs):
    parts, o_ref = refs[:-1], refs[-1]
    length, half = other_ref.shape
    here = heads // 2
    core = info_ref[0]
    gates = jax.nn.sigmoid(gate_ref[...][:, 2 * heads : 3 * heads])
    results, _ = blend(parts, length, here, head_dim)
    for side, normed_ref in enumerate((low_ref, high_ref)):
        for head in range(here):
            cols = slice(head * head_dim, (head + 1) * head_dim)
            place = side * here + head
            value = jnp.where(core == side, results[head], other_ref[:, cols].astype(F32))
            o_ref[:, place * head_dim : (place + 1) * head_dim] = (
                normed_ref[:, cols] + gates[:, place : place + 1] * value
            ).astype(BF16)


def finish(info, low, high, gates, other, parts, head_dim, heads):
    return pl.pallas_call(
        functools.partial(final_kernel, head_dim, heads),
        out_shape=jax.ShapeDtypeStruct((low.shape[0], 2 * low.shape[1]), BF16),
        in_specs=[pl.BlockSpec(memory_space=pltpu.SMEM)]
        + [pl.BlockSpec(memory_space=pltpu.VMEM)] * (4 + len(parts)),
        name="finish",
    )(info, low, high, gates, other, *parts)


def per_device(
    tokens,
    owners,
    entries,
    store,
    mixer_query_weight,
    mixer_key_weight,
    mixer_value_weight,
    strength_weight,
    decay_weight,
    head_decay_rate,
    extra_forgetting_exponent,
    output_norm_gain,
    retrieval_query_weight,
    passage_key_weight,
    passage_value_weight,
    retrieval_gate_weight,
):
    heads = head_decay_rate.shape[0]
    head_dim = output_norm_gain.shape[0]
    length = tokens.shape[0]
    devices = lax.axis_size("st")
    chips = devices // 2
    blocks = owners.shape[0]
    passage_rows = store.shape[1]
    half = heads * head_dim // 2
    me = lax.axis_index("st")
    core, chip = me % 2, me // 2
    swap = [(i, i ^ 1) for i in range(devices)]
    right = [(i, (i + 2) % devices) for i in range(devices)]
    left = [(i, (i - 2) % devices) for i in range(devices)]
    send = lambda array, pairs: lax.ppermute(array, "st", pairs)

    def project(rows, weight):
        return jnp.dot(rows, weight, preferred_element_type=F32).astype(BF16)

    wants = lax.all_gather(owners * store.shape[0] + entries, "st", axis=0, tiled=True)
    wants, tokens = lax.optimization_barrier((wants, tokens))
    info = jnp.stack([core, me]).astype(jnp.int32)

    rquery = project(tokens, retrieval_query_weight)
    q_own = lax.dynamic_slice_in_dim(rquery, core * half, half, 1)
    q_sib = send(lax.dynamic_slice_in_dim(rquery, (1 - core) * half, half, 1), swap)

    reach = chips // 2
    from_left, from_right = [(q_own, q_sib)], [(q_own, q_sib)]
    for hop in range(1, reach):
        from_left.append(tuple(send(part, right) for part in from_left[-1]))
        from_right.append(tuple(send(part, left) for part in from_right[-1]))
    far_own = send(from_left[-1][0], right)
    far_sib = send(from_right[-1][1], left)

    flat_store = store.reshape(-1, store.shape[2])
    keys = project(flat_store, passage_key_weight)
    values = project(flat_store, passage_value_weight)
    away = (1 - core) * half
    pair_sib = send(
        jnp.concatenate(
            [
                lax.dynamic_slice_in_dim(keys, away, half, 1),
                lax.dynamic_slice_in_dim(values, away, half, 1),
            ],
            axis=1,
        ),
        swap,
    )
    q = project(tokens, mixer_query_weight)
    k = project(tokens, mixer_key_weight)
    v = project(tokens, mixer_value_weight)
    small = jnp.concatenate([strength_weight, decay_weight, retrieval_gate_weight], axis=1)
    gates = jnp.dot(tokens, small, preferred_element_type=F32)

    def attended(units, offsets):
        return attend(
            units, offsets, wants, info, keys, values, pair_sib, head_dim, passage_rows, chips
        )

    here = attended(list(from_left[0]), [(0, False), (0, True)])
    to_left, to_right = {}, {}
    for hop in range(1, reach):
        res = attended(
            list(from_left[hop]) + list(from_right[hop]),
            [(-hop, False), (-hop, True), (hop, False), (hop, True)],
        )
        to_left[hop], to_right[hop] = res[:2], res[2:]
    far = attended([far_own, far_sib], [(reach, False), (reach, True)])

    pack = min(4 * BLOCK_TOKENS, length)

    def mixer(group, after):
        held = lax.optimization_barrier((q, k, v, *after))
        return delta(
            *held[:3], gates, extra_forgetting_exponent, head_decay_rate, output_norm_gain,
            pack, group, 2,
        )

    low = mixer(0, far)

    going_right, going_left = [far[0], None], [None, far[1]]
    for hop in range(reach - 1, 0, -1):
        for going, pairs, mine in (
            (going_right, right, to_right[hop]),
            (going_left, left, to_left[hop]),
        ):
            for part in range(2):
                if going[part] is None:
                    going[part] = mine[part]
                else:
                    came = send(going[part], pairs)
                    came, low = lax.optimization_barrier((came, low))
                    going[part] = merge([came, mine[part]], length, head_dim)
    high = mixer(1, [going_right[0], going_left[1]])
    ends = [
        [here[part]] + [send(going_right[part], right), send(going_left[part], left)]
        for part in range(2)
    ]
    ends, high = lax.optimization_barrier((ends, high))
    other = send(merge(ends[1], length, head_dim, final=True), swap)
    return finish(info, low, high, gates, other, ends[0], head_dim, heads)


def solution(mesh):
    rows = ("grp", "st")
    return jax.shard_map(
        per_device,
        mesh=mesh,
        in_specs=(
            P(rows, None),
            P(rows, None),
            P(rows, None),
            P(rows, None, None),
            P(None, "tp"),
            P(None, "tp"),
            P(None, "tp"),
            P(None, "tp"),
            P(None, "tp"),
            P("tp"),
            P(rows, "tp"),
            P(),
            P(None, "tp"),
            P(None, "tp"),
            P(None, "tp"),
            P(None, "tp"),
        ),
        out_specs=P(rows, "tp"),
        check_vma=False,
    )
```

```python
import functools

import jax
import jax.numpy as jnp
from jax import lax
from jax.experimental import pallas as pl
from jax.experimental.pallas import tpu as pltpu
from jax.sharding import PartitionSpec as P

BLOCK_TOKENS = 64
EPS = 1e-06
MISSING = -1e30
WANT_ROWS = 16
F32 = jnp.float32
BF16 = jnp.bfloat16


def dot_nt(left, right):
    return lax.dot_general(left, right, (((1,), (1,)), ((), ())), preferred_element_type=F32)


def dot_tn(left, right):
    return lax.dot_general(left, right, (((0,), (0,)), ((), ())), preferred_element_type=F32)


def dot_nn(left, right):
    return jnp.dot(left.astype(BF16), right.astype(BF16), preferred_element_type=F32)


def attend_kernel(
    units, head_dim, passage_rows, blocks, want_ref, info_ref, *refs
):
    queries = refs[:units]
    k_own, v_own, k_sib, v_sib = refs[units : units + 4]
    outs = refs[units + 4 :]
    length, half = queries[0].shape[0] - WANT_ROWS, queries[0].shape[1]
    heads = half // head_dim
    width = want_ref.shape[1] // blocks
    scale = head_dim ** (-0.5)
    core, me = info_ref[0], info_ref[1]
    sibling = me + 1 - 2 * core

    def find(named, device):
        hit = jnp.int32(0)
        for owner, entry in named:
            hit = jnp.where(owner == device, entry + 1, hit)
        row = pl.multiple_of(jnp.maximum(hit - 1, 0) * passage_rows, passage_rows)
        return row, jnp.where(hit > 0, 0.0, MISSING).astype(F32)

    nothing = jnp.zeros((BLOCK_TOKENS, head_dim), BF16)
    for unit in range(units):
        q_ref, o_ref = queries[unit], outs[unit]
        stats = []
        for block in range(blocks):
            named = [
                (
                    want_ref[2 * unit, block * width + place],
                    want_ref[2 * unit + 1, block * width + place],
                )
                for place in range(width)
            ]
            row_own, bias_own = find(named, me)
            row_sib, bias_sib = find(named, sibling)
            rows = slice(block * BLOCK_TOKENS, (block + 1) * BLOCK_TOKENS)
            query = q_ref[rows, :]
            spread = jnp.concatenate(
                [
                    jnp.concatenate(
                        [
                            query[:, head * head_dim : (head + 1) * head_dim]
                            if head == place
                            else nothing
                            for place in range(heads)
                        ],
                        axis=1,
                    )
                    for head in range(heads)
                ],
                axis=0,
            )
            keys = jnp.concatenate(
                [k_own[pl.ds(row_own, passage_rows), :], k_sib[pl.ds(row_sib, passage_rows), :]],
                axis=0,
            )
            values = jnp.concatenate(
                [v_own[pl.ds(row_own, passage_rows), :], v_sib[pl.ds(row_sib, passage_rows), :]],
                axis=0,
            )
            scores = dot_nt(keys, spread) * scale
            own, sib = scores[:passage_rows] + bias_own, scores[passage_rows:] + bias_sib
            peak = jnp.max(jnp.maximum(own, sib), axis=0, keepdims=True)
            e_own = jnp.exp(own - peak)
            e_sib = jnp.exp(sib - peak)
            total = jnp.sum(e_own + e_sib, axis=0, keepdims=True)
            inv = 1.0 / total
            weights = jnp.concatenate([e_own * inv, e_sib * inv], axis=0).astype(BF16)
            result = dot_tn(weights, values)
            lse = peak + jnp.log(total)
            for head in range(heads):
                cols = slice(head * head_dim, (head + 1) * head_dim)
                span = slice(head * BLOCK_TOKENS, (head + 1) * BLOCK_TOKENS)
                o_ref[rows, cols] = result[span, cols].astype(BF16)
            stats.append(
                jnp.concatenate(
                    [
                        lse[:, head * BLOCK_TOKENS : (head + 1) * BLOCK_TOKENS]
                        for head in range(heads)
                    ],
                    axis=0,
                )
            )
        store_stats(o_ref, jnp.concatenate(stats, axis=1), length)


def store_stats(o_ref, lse, length):
    heads = lse.shape[0]
    width = o_ref.shape[1]
    high = lse.astype(BF16).astype(F32)
    mid = (lse - high).astype(BF16).astype(F32)
    low = lse - high - mid
    pad = jnp.zeros((16 - 3 * heads, length), F32)
    pieces = jnp.concatenate([high, mid, low, pad], axis=0).astype(BF16)
    for part in range(length // width):
        o_ref[length + 16 * part : length + 16 * (part + 1), :] = pieces[
            :, part * width : (part + 1) * width
        ]


def load_stats(ref, length, heads):
    width = ref.shape[1]
    parts = [
        ref[length + 16 * part : length + 16 * (part + 1), :].astype(F32)
        for part in range(length // width)
    ]
    pieces = jnp.concatenate(parts, axis=1)
    return pieces[:heads] + pieces[heads : 2 * heads] + pieces[2 * heads : 3 * heads]


def blend(refs, length, heads, head_dim):
    stats = [load_stats(ref, length, heads) for ref in refs]
    peak = functools.reduce(jnp.maximum, stats)
    expo = [jnp.exp(stat - peak) for stat in stats]
    total = functools.reduce(jnp.add, expo)
    inv = 1.0 / total
    lse = peak + jnp.log(total)
    shares = [
        jnp.transpose(jnp.concatenate([e * inv] + [jnp.zeros((8 - heads, length), F32)], axis=0))
        for e in expo
    ]
    results = []
    for head in range(heads):
        cols = slice(head * head_dim, (head + 1) * head_dim)
        results.append(
            functools.reduce(
                jnp.add,
                [
                    ref[:length, cols].astype(F32) * share[:, head : head + 1]
                    for ref, share in zip(refs, shares)
                ],
            )
        )
    return results, lse


def merge_kernel(length, head_dim, final, *refs):
    inputs, o_ref = refs[:-1], refs[-1]
    heads = o_ref.shape[1] // head_dim
    results, lse = blend(inputs, length, heads, head_dim)
    for head, result in enumerate(results):
        o_ref[:length, head * head_dim : (head + 1) * head_dim] = result.astype(BF16)
    if not final:
        store_stats(o_ref, lse, length)


def merge(parts, length, head_dim, final=False):
    shape = (length, parts[0].shape[1]) if final else parts[0].shape
    return pl.pallas_call(
        functools.partial(merge_kernel, length, head_dim, final),
        out_shape=jax.ShapeDtypeStruct(shape, BF16),
        cost_estimate=pl.CostEstimate(flops=2_000_000, bytes_accessed=3_000_000, transcendentals=0),
        name="merge",
    )(*parts)


def attend(units, requests, info, keys, values, pair_sib, head_dim, passage_rows):
    length, half = units[0].shape[0] - WANT_ROWS, units[0].shape[1]
    blocks = length // BLOCK_TOKENS
    wants = jnp.concatenate(
        [unit[length : length + 2, :requests] for unit in units], axis=0
    ).astype(jnp.int32)
    rows = keys.shape[0]
    packed = length + 16 * (length // half)
    whole = lambda shape: pl.BlockSpec(shape, lambda i, w, c: (0, 0))
    mine = pl.BlockSpec((rows, half), lambda i, w, c: (0, c[0]))
    second = pl.BlockSpec((rows, half), lambda i, w, c: (0, 1))
    return pl.pallas_call(
        functools.partial(
            attend_kernel, len(units), head_dim, passage_rows, blocks
        ),
        out_shape=[jax.ShapeDtypeStruct((packed, half), BF16)] * len(units),
        grid_spec=pltpu.PrefetchScalarGridSpec(
            num_scalar_prefetch=2,
            grid=(1,),
            in_specs=[whole((length + WANT_ROWS, half))] * len(units)
            + [mine, mine, whole((rows, half)), second],
            out_specs=[whole((packed, half))] * len(units),
        ),
        cost_estimate=pl.CostEstimate(
            flops=1_500_000_000 * len(units), bytes_accessed=4_000_000, transcendentals=0
        ),
        name="attend",
    )(wants, info, *units, keys, values, pair_sib, pair_sib)


def delta_kernel(pack, chunk, first, q_ref, k_ref, v_ref, gate_ref, extra_ref, rate_ref, gain_ref, o_ref):
    length, width = q_ref.shape
    head_dim = gain_ref.shape[1]
    heads = width // head_dim
    packs = length // pack
    scale = head_dim ** (-0.5)
    row = lax.broadcasted_iota(jnp.int32, (pack, pack), 0)
    col = lax.broadcasted_iota(jnp.int32, (pack, pack), 1)
    same = (row // chunk) == (col // chunk)
    lower = same & (row >= col)
    strict = same & (row > col)
    ident = jnp.where(row == col, 1.0, 0.0).astype(F32)
    tri = jnp.where(lower, 1.0, 0.0).astype(F32)
    tail = jnp.where(same, 1.0, 0.0).astype(F32)
    gates = gate_ref[...]
    every = rate_ref.shape[1]
    beta_all = jax.nn.sigmoid(gates[:, first : first + heads])
    raw = gates[:, every + first : every + first + heads]
    softplus = jnp.maximum(raw, 0.0) + jnp.log1p(jnp.exp(-jnp.abs(raw)))
    mine = slice(first, first + heads)
    decay_all = -rate_ref[:, mine] * softplus + extra_ref[:, mine]
    gain = gain_ref[...]
    work = []
    for half in range(packs):
        rows = slice(half * pack, (half + 1) * pack)
        decay = jnp.concatenate([decay_all[rows], jnp.zeros((pack, 128 - heads), F32)], axis=1)
        cum = jnp.dot(tri, decay, precision=lax.Precision.HIGHEST, preferred_element_type=F32)
        ends = jnp.dot(tail, decay, precision=lax.Precision.HIGHEST, preferred_element_type=F32)
        cum_t = jnp.transpose(cum)
        for head in range(heads):
            cols = slice(head * head_dim, (head + 1) * head_dim)
            q, k, v = q_ref[rows, cols], k_ref[rows, cols], v_ref[rows, cols]
            q32, k32 = q.astype(F32), k.astype(F32)
            qn = q32 * (lax.rsqrt(jnp.sum(q32 * q32, axis=1, keepdims=True) + EPS) * scale)
            kn = k32 * lax.rsqrt(jnp.sum(k32 * k32, axis=1, keepdims=True) + EPS)
            beta = beta_all[rows, head : head + 1]
            c_col = cum[:, head : head + 1]
            spread = c_col - cum_t[head : head + 1, :]
            damp = jnp.where(lower, jnp.exp(jnp.where(lower, spread, 0.0)), 0.0)
            kb = kn.astype(BF16)
            inner = jnp.where(strict, dot_nt(kb, kb) * damp * beta, 0.0)
            within = (dot_nt(qn.astype(BF16), kb) * damp).astype(BF16)
            inverse = ident
            size = 1
            while size < chunk:
                cut = ((row // (2 * size)) == (col // (2 * size))) & ((row // size) != (col // size))
                piece = jnp.where(cut, inner, 0.0)
                if size == 1:
                    inverse = ident - piece
                else:
                    inverse = inverse - dot_nn(dot_nn(inverse, piece), inverse)
                size *= 2
            grow = jnp.exp(c_col)
            sides = jnp.concatenate([v.astype(F32) * beta, kn * (beta * grow)], axis=1)
            mixed = dot_nn(inverse, sides)
            base, key_mix = mixed[:, :head_dim], mixed[:, head_dim:]
            q_dec = qn * grow
            k_tail = kn * jnp.exp(ends[:, head : head + 1] - c_col)
            work.append(
                (
                    base,
                    key_mix.astype(BF16),
                    q_dec.astype(BF16),
                    jnp.transpose(k_tail).astype(BF16),
                    within,
                    jnp.exp(ends[:, head : head + 1]),
                )
            )
    state = [jnp.zeros((head_dim, head_dim), F32) for _ in range(heads)]
    for half in range(packs):
        fresh_parts = [[] for _ in range(heads)]
        cross_parts = [[] for _ in range(heads)]
        for step in range(pack // chunk):
            rows = slice(step * chunk, (step + 1) * chunk)
            for head in range(heads):
                base, key_mix, q_dec, k_tail, _, carry = work[half * heads + head]
                stacked = jnp.concatenate([key_mix[rows], q_dec[rows]], axis=0)
                read = jnp.dot(stacked, state[head].astype(BF16), preferred_element_type=F32)
                fresh = (base[rows] - read[:chunk]).astype(BF16)
                cross_parts[head].append(read[chunk:])
                fresh_parts[head].append(fresh)
                kept = carry[step * chunk : step * chunk + 1, :]
                state[head] = state[head] * kept + jnp.dot(
                    k_tail[:, rows], fresh, preferred_element_type=F32
                )
        for head in range(heads):
            within = work[half * heads + head][4]
            result = jnp.concatenate(cross_parts[head], axis=0) + jnp.dot(
                within, jnp.concatenate(fresh_parts[head], axis=0), preferred_element_type=F32
            )
            norm = lax.rsqrt(jnp.mean(result * result, axis=1, keepdims=True) + EPS)
            o_ref[half * pack : (half + 1) * pack, head * head_dim : (head + 1) * head_dim] = (
                result * norm * gain
            )


def delta(q, k, v, gates, extra, rate, gain, pack, group, groups):
    length, width = q.shape
    half = width // groups
    first = group * (rate.shape[0] // groups)
    part = pl.BlockSpec((length, half), lambda i: (0, group))
    whole = lambda array: pl.BlockSpec(array.shape, lambda i: (0, 0))
    rate, gain = rate[None, :], gain[None, :]
    return pl.pallas_call(
        functools.partial(delta_kernel, pack, BLOCK_TOKENS, first),
        out_shape=jax.ShapeDtypeStruct((length, half), F32),
        grid=(1,),
        in_specs=[part, part, part, whole(gates), whole(extra), whole(rate), whole(gain)],
        out_specs=pl.BlockSpec((length, half), lambda i: (0, 0)),
        cost_estimate=pl.CostEstimate(
            flops=8_000_000_000, bytes_accessed=2_000_000, transcendentals=0
        ),
        name="delta",
    )(q, k, v, gates, extra, rate, gain)


def final_kernel(head_dim, heads, info_ref, low_ref, high_ref, gate_ref, other_ref, *refs):
    parts, o_ref = refs[:-1], refs[-1]
    length, half = other_ref.shape
    here = heads // 2
    core = info_ref[0]
    gates = jax.nn.sigmoid(gate_ref[...][:, 2 * heads : 3 * heads])
    results, _ = blend(parts, length, here, head_dim)
    for side, normed_ref in enumerate((low_ref, high_ref)):
        for head in range(here):
            cols = slice(head * head_dim, (head + 1) * head_dim)
            place = side * here + head
            value = jnp.where(core == side, results[head], other_ref[:, cols].astype(F32))
            o_ref[:, place * head_dim : (place + 1) * head_dim] = (
                normed_ref[:, cols] + gates[:, place : place + 1] * value
            ).astype(BF16)


def finish(info, low, high, gates, other, parts, head_dim, heads):
    return pl.pallas_call(
        functools.partial(final_kernel, head_dim, heads),
        out_shape=jax.ShapeDtypeStruct((low.shape[0], 2 * low.shape[1]), BF16),
        in_specs=[pl.BlockSpec(memory_space=pltpu.SMEM)]
        + [pl.BlockSpec(memory_space=pltpu.VMEM)] * (4 + len(parts)),
        name="finish",
    )(info, low, high, gates, other, *parts)


def per_device(
    tokens,
    owners,
    entries,
    store,
    mixer_query_weight,
    mixer_key_weight,
    mixer_value_weight,
    strength_weight,
    decay_weight,
    head_decay_rate,
    extra_forgetting_exponent,
    output_norm_gain,
    retrieval_query_weight,
    passage_key_weight,
    passage_value_weight,
    retrieval_gate_weight,
):
    heads = head_decay_rate.shape[0]
    head_dim = output_norm_gain.shape[0]
    length = tokens.shape[0]
    devices = lax.axis_size("st")
    chips = devices // 2
    blocks = owners.shape[0]
    passage_rows = store.shape[1]
    half = heads * head_dim // 2
    me = lax.axis_index("st")
    core, chip = me % 2, me // 2
    swap = [(i, i ^ 1) for i in range(devices)]
    right = [(i, (i + 2) % devices) for i in range(devices)]
    left = [(i, (i - 2) % devices) for i in range(devices)]
    send = lambda array, pairs: lax.ppermute(array, "st", pairs)

    def project(rows, weight):
        return jnp.dot(rows, weight, preferred_element_type=F32).astype(BF16)

    info = jnp.stack([core, me]).astype(jnp.int32)
    requests = owners.size
    wants = jnp.stack([owners.reshape(requests), entries.reshape(requests)]).astype(BF16)
    wants = jnp.pad(wants, ((0, WANT_ROWS - 2), (0, half - requests)))

    rquery = project(tokens, retrieval_query_weight)

    def packed_queries(side):
        return jnp.concatenate([lax.dynamic_slice_in_dim(rquery, side * half, half, 1), wants], 0)

    q_own = packed_queries(core)
    q_sib = send(packed_queries(1 - core), swap)

    reach = chips // 2
    from_left, from_right = [(q_own, q_sib)], [(q_own, q_sib)]
    for hop in range(1, reach):
        from_left.append(tuple(send(part, right) for part in from_left[-1]))
        from_right.append(tuple(send(part, left) for part in from_right[-1]))
    far_own = send(from_left[-1][0], right)
    far_sib = send(from_right[-1][1], left)

    flat_store = store.reshape(-1, store.shape[2])
    keys = project(flat_store, passage_key_weight)
    values = project(flat_store, passage_value_weight)
    away = (1 - core) * half
    pair_sib = send(
        jnp.concatenate(
            [
                lax.dynamic_slice_in_dim(keys, away, half, 1),
                lax.dynamic_slice_in_dim(values, away, half, 1),
            ],
            axis=1,
        ),
        swap,
    )
    q = project(tokens, mixer_query_weight)
    k = project(tokens, mixer_key_weight)
    v = project(tokens, mixer_value_weight)
    small = jnp.concatenate([strength_weight, decay_weight, retrieval_gate_weight], axis=1)
    gates = jnp.dot(tokens, small, preferred_element_type=F32)

    def attended(units):
        return attend(
            units, requests, info, keys, values, pair_sib, head_dim, passage_rows
        )

    here = attended(list(from_left[0]))
    to_left, to_right = {}, {}
    for hop in range(1, reach):
        res = attended(list(from_left[hop]) + list(from_right[hop]))
        to_left[hop], to_right[hop] = res[:2], res[2:]
    far = attended([far_own, far_sib])

    pack = min(4 * BLOCK_TOKENS, length)

    def mixer(group, after):
        held = lax.optimization_barrier((q, k, v, *after))
        return delta(
            *held[:3], gates, extra_forgetting_exponent, head_decay_rate, output_norm_gain,
            pack, group, 2,
        )

    low = mixer(0, far)

    going_right, going_left = [far[0], None], [None, far[1]]
    for hop in range(reach - 1, 0, -1):
        for going, pairs, mine in (
            (going_right, right, to_right[hop]),
            (going_left, left, to_left[hop]),
        ):
            for part in range(2):
                if going[part] is None:
                    going[part] = mine[part]
                else:
                    came = send(going[part], pairs)
                    came, low = lax.optimization_barrier((came, low))
                    going[part] = merge([came, mine[part]], length, head_dim)
    high = mixer(1, [going_right[0], going_left[1]])
    ends = [
        [here[part]] + [send(going_right[part], right), send(going_left[part], left)]
        for part in range(2)
    ]
    ends, high = lax.optimization_barrier((ends, high))
    other = send(merge(ends[1], length, head_dim, final=True), swap)
    return finish(info, low, high, gates, other, ends[0], head_dim, heads)


def solution(mesh):
    rows = ("grp", "st")
    return jax.shard_map(
        per_device,
        mesh=mesh,
        in_specs=(
            P(rows, None),
            P(rows, None),
            P(rows, None),
            P(rows, None, None),
            P(None, "tp"),
            P(None, "tp"),
            P(None, "tp"),
            P(None, "tp"),
            P(None, "tp"),
            P("tp"),
            P(rows, "tp"),
            P(),
            P(None, "tp"),
            P(None, "tp"),
            P(None, "tp"),
            P(None, "tp"),
        ),
        out_specs=P(rows, "tp"),
        check_vma=False,
    )
```
